32 devices in a mesh: ep: 16 (over z, y, x), tp: 2 (over core).
Axes of the slice: x: 2, y: 2, z: 4, core: 2. Of those that a mesh axis runs over, the one named last changes fastest.
Arguments:
- tokens: bfloat16 [512, 4096], P('ep', 'tp')
- norm_gain: float32 [4096], P('tp'), may hold values from 0.1 to 1.9
- routes: int32 [512, 8], P('ep'), may hold values from 0 to 15, all different within a row; in each aligned block of 32 rows (0 to 31, 32 to 63, ...) at most 24 rows name the same one
- route_weights: float32 [512, 8], P('ep'), may hold values from 0.1 to 1
- gate_proj: bfloat16 [16, 4096, 1024], P('ep', 'tp'), may hold values from -0.09375 to 0.09375
- up_proj: bfloat16 [16, 4096, 1024], P('ep', 'tp'), may hold values from -0.09375 to 0.09375
- down_proj: bfloat16 [16, 1024, 4096], P('ep', None, 'tp')
- shared_gate: bfloat16 [4096, 1024], P('tp'), may hold values from -0.09375 to 0.09375
- shared_up: bfloat16 [4096, 1024], P('tp'), may hold values from -0.09375 to 0.09375
- shared_down: bfloat16 [1024, 4096], P(None, 'tp')
- out_gain: float32 [4096], P('tp'), may hold values from 0.1 to 1.9
Outputs:
- mixed_out: bfloat16 [512, 4096], P('ep', 'tp')
The draws below stay inside these ranges and needn't reach their ends.
Inputs may be any that keep to these rules, and one draw needn't show every extreme that they name: `routes`: among the 32 rows of one device no expert is named more than 24 times, and in every draw some expert is named exactly 24 times by the rows of some device.
All inputs are finite; a program needn't handle non-finite values.
Results may differ from the reference program's by a relative error of at most 0.028.
Values may be sent and summed in bfloat16 or wider, within the bound.
A program may use at most 64 MiB of HBM per device.

```python
import math
import jax
import jax.numpy as jnp
import numpy as np
from jax import lax

D = 4096
F = 1024
FS = 1024
TOP_K = 8
TOK_DEV = 32
EXPERTS = 16
CAP = 24
TOKENS = 512
N_EP = 16
N_TP = 2


def column_scales(key, length):
    rising = jnp.exp(jnp.linspace(0.0, math.log(6.0), length))
    return rising * jax.random.uniform(key, (length,), jnp.float32, 0.5, 1.5)


def draw_tokens(key, part):
    key_base = jax.random.fold_in(key, 11)
    key_rows = jax.random.fold_in(key, 12)
    key_cols = jax.random.fold_in(key, 13)
    values = jax.random.normal(key_base, (TOKENS, D), jnp.float32)
    row_scale = jnp.exp(jax.random.uniform(key_rows, (TOKENS, 1), jnp.float32, 0.0, math.log(10.0)))
    return (values * row_scale * column_scales(key_cols, D)[None, :]).astype(jnp.bfloat16)


def down_values(key, shape):
    key_base = jax.random.fold_in(key, 21)
    key_cols = jax.random.fold_in(key, 22)
    values = jax.random.normal(key_base, shape, jnp.float32)
    return values * shape[-2] ** (-0.5) * column_scales(key_cols, D)


def draw_down_proj(key, part):
    return down_values(key, (EXPERTS, F, D)).astype(jnp.bfloat16)


def draw_shared_down(key, part):
    return down_values(key, (FS, D)).astype(jnp.bfloat16)


def block_scale(own_key, shape, cuts, least, largest):
    level, own = 1.0, jax.random.fold_in(own_key, 6)
    for dim, blocks in cuts:
        heights = jnp.exp(jax.random.uniform(jax.random.fold_in(own, dim), (blocks,), jnp.float32, least / len(cuts), largest / len(cuts)))
        level = level * jnp.repeat(heights, shape[dim] // blocks).reshape([-1 if axis == dim else 1 for axis in range(len(shape))])
    return level


def shared_out(own_key, own, number, rows, count, top, most, lean):
    order = jax.random.permutation(own_key, count)
    packed, usual = load_shares(count, rows * top, most, lean, True), load_shares(count, rows * top, most, lean, False)
    places = jnp.arange(count)

    def named(sizes, rotation):
        used = int((sizes > 0).sum())
        fixed = max(1, used // 4)
        moved = fixed + (places - fixed + rotation * (used - fixed)) % max(1, count - fixed)
        return jnp.zeros((count,), jnp.int32).at[order[jnp.where(places < fixed, places, moved)]].set(jnp.asarray(sizes, jnp.int32))

    sizes = jnp.where(number % 4 == 0, named(packed, number // 4), named(usual, number - number // 4 - 1))
    mixed = jax.random.permutation(jax.random.fold_in(own, 3), count)
    giver, receiver = mixed[0:count // 2 * 2:2], mixed[1:count // 2 * 2:2]
    margin = jnp.minimum(sizes[giver] - 1, most - sizes[receiver]) // 2
    margin = jnp.where((giver == order[0]) | (receiver == order[0]) | (sizes[receiver] == 0), 0, jnp.maximum(margin, 0))
    moved = jax.random.randint(jax.random.fold_in(own, 4), (count // 2,), 0, 1 << 20) % (margin + 1)
    sizes = sizes.at[giver].add(-moved).at[receiver].add(moved)
    items = jnp.searchsorted(jnp.cumsum(sizes), jnp.arange(rows * top), side="right").astype(jnp.int32)
    table = items.reshape(top, rows).T
    table = table[jax.random.permutation(jax.random.fold_in(own, 1), rows)]
    rotation = jax.random.randint(jax.random.fold_in(own, 2), (rows, 1), 0, top)
    return jnp.take_along_axis(table, (jnp.arange(top)[None, :] + rotation) % top, axis=1)


def load_shares(number_of, total, bound, lean, full):
    weights = [(1 << 20) // math.isqrt(grade ** lean) + 1 for grade in range(1, number_of + 1)]
    largest = bound if full else min(bound, max(-(-total // number_of), total * weights[0] // sum(weights)))
    least = 1 if total - largest >= number_of - 1 else 0
    counts, surplus = [largest] + [least] * (number_of - 1), total - largest - least * (number_of - 1)
    while surplus > 0:
        free = [i for i in range(1, number_of) if counts[i] < largest] or [i for i in range(1, number_of) if counts[i] < bound]
        whole, budget = sum([weights[i] for i in free]), surplus
        for i in free:
            addition = min(bound - counts[i], max(1, budget * weights[i] // whole), surplus)
            counts[i] = counts[i] + addition
            surplus = surplus - addition
    return np.array(counts)


def bell_draw(key, shape, width, most, shards=(), kind=jnp.bfloat16):
    array = jax.random.normal(key, shape, jnp.float32) * width
    if len(shards) > 0:
        array = block_scale(key, shape, shards, -0.22, 0.18) * array
    return jnp.clip(array, min=-most, max=most).astype(kind)


def setup_inputs(seed: int = 0) -> dict:
    streams_of = jax.random.split(jax.random.key(seed), 12)
    tokens = draw_tokens(jax.random.fold_in(streams_of[11], 71), 0)
    norm_gain = jnp.clip(1.0 + 0.18 * jax.random.normal(streams_of[1], (D,), jnp.float32), 0.1, 1.9)
    routes_keys = jax.random.split(jax.random.fold_in(streams_of[2], 1), TOKENS // TOK_DEV)
    routes_turns = jax.random.permutation(jax.random.fold_in(streams_of[2], 3), TOKENS // TOK_DEV)
    routes = jax.vmap(lambda own, number: shared_out(jax.random.fold_in(streams_of[2], 2), own, number, TOK_DEV, EXPERTS, TOP_K, CAP, 2))(routes_keys, routes_turns).reshape((TOKENS, TOP_K))
    route_weights = jnp.clip(jnp.exp(math.log(1.0) - 2.3025851 * jax.random.uniform(streams_of[3], (TOKENS, TOP_K), jnp.float32) ** block_scale(streams_of[3], (TOKENS, TOP_K), ((0, 16),), -0.2, 0.2)), 0.1, 1.0)
    gate_proj = bell_draw(streams_of[4], (EXPERTS, D, F), D ** -0.5, 0.09375, ((0, 16), (1, 2)))
    up_proj = bell_draw(streams_of[5], (EXPERTS, D, F), D ** -0.5, 0.09375, ((0, 16), (1, 2)))
    down_proj = draw_down_proj(jax.random.fold_in(streams_of[11], 71), 0)
    shared_gate = bell_draw(streams_of[7], (D, FS), D ** -0.5, 0.09375, ((0, 2),))
    shared_up = bell_draw(streams_of[8], (D, FS), D ** -0.5, 0.09375, ((0, 2),))
    shared_down = draw_shared_down(jax.random.fold_in(streams_of[11], 71), 0)
    out_gain = jnp.clip(1.0 + 0.18 * jax.random.normal(streams_of[10], (D,), jnp.float32), 0.1, 1.9)
    return {"tokens": tokens, "norm_gain": norm_gain, "routes": routes, "route_weights": route_weights, "gate_proj": gate_proj, "up_proj": up_proj, "down_proj": down_proj, "shared_gate": shared_gate, "shared_up": shared_up, "shared_down": shared_down, "out_gain": out_gain}


def split_product(left_rows, weight):
    row_count = left_rows.shape[0]
    out_width = weight.shape[1]
    left_side = left_rows.astype(jnp.float32).reshape(row_count, N_TP, D // N_TP)
    right_side = weight.astype(jnp.float32).reshape(N_TP, D // N_TP, out_width)
    partial_value = jnp.einsum('rtd,tdf->rtf', left_side, right_side).astype(jnp.bfloat16)
    partial_value = lax.optimization_barrier(partial_value).astype(jnp.float32)
    return lax.optimization_barrier(jnp.sum(partial_value, axis=1))

def swiglu(gate_pre, up_pre):
    return (jax.nn.silu(gate_pre) * up_pre).astype(jnp.bfloat16)

def reference(tokens, norm_gain, routes, route_weights, gate_proj, up_proj, down_proj, shared_gate, shared_up, shared_down, out_gain):
    tokens_f = tokens.astype(jnp.float32)
    scale = lax.rsqrt(lax.optimization_barrier(jnp.mean(tokens_f * tokens_f, axis=1, keepdims=True)) + 1e-06)
    normed = (tokens_f * scale * norm_gain[None, :]).astype(jnp.bfloat16)
    shared_hidden = swiglu(split_product(normed, shared_gate), split_product(normed, shared_up))
    shared_part = jnp.dot(shared_hidden, shared_down, preferred_element_type=jnp.float32)
    chosen = jnp.concatenate([routes.reshape(-1), jnp.full((1,), -1, jnp.int32)])
    weight_list = jnp.concatenate([route_weights.reshape(-1), jnp.zeros((1,), jnp.float32)])
    token_list = jnp.concatenate([jnp.arange(TOKENS * TOP_K, dtype=jnp.int32) // TOP_K, jnp.zeros((1,), jnp.int32)])
    row_limit = N_EP * CAP
    sentinel = TOKENS * TOP_K

    def add_expert(totals, expert):
        picked = jnp.nonzero(chosen == expert, size=row_limit, fill_value=sentinel)[0].astype(jnp.int32)
        rows_of = token_list[picked]
        chosen_rows = normed[rows_of]
        hidden = swiglu(split_product(chosen_rows, gate_proj[expert]), split_product(chosen_rows, up_proj[expert]))
        result = jnp.dot(hidden, down_proj[expert], preferred_element_type=jnp.float32).astype(jnp.bfloat16)
        result = lax.optimization_barrier(result).astype(jnp.float32)
        totals = totals.at[rows_of].add(result * weight_list[picked][:, None])
        return (totals, None)
    routed, _ = lax.scan(add_expert, jnp.zeros((TOKENS, D), jnp.float32), jnp.arange(EXPERTS, dtype=jnp.int32))
    mixed = shared_part + routed
    final_scale = lax.rsqrt(lax.optimization_barrier(jnp.mean(mixed * mixed, axis=1, keepdims=True)) + 1e-06)
    return (mixed * final_scale * out_gain[None, :]).astype(jnp.bfloat16)
```

```python
import functools

import jax
import jax.numpy as jnp
from jax import lax
from jax.experimental import pallas as pl
from jax.experimental.pallas import tpu as pltpu
from jax.sharding import PartitionSpec as P


F32 = jnp.float32
BF16 = jnp.bfloat16


def layer_kernel(
    zs,
    tokens_ref,
    gain_ref,
    routes_ref,
    rw_ref,
    out_gain_ref,
    gate_hbm,
    up_hbm,
    down_hbm,
    sgate_hbm,
    sup_hbm,
    sdown_hbm,
    out_ref,
    wg,
    wu,
    wd,
    sg,
    su,
    sd,
    slab,
    gu_s,
    gu_r,
    sh_s,
    sh_r,
    ss_s,
    ss_r,
    sbuf,
    rbuf,
    sz,
    rz,
    acc_x,
    acc_y,
    acc_o,
    obuf,
    shared_out,
    hid,
    w_sem,
    ag_send,
    ag_recv,
    rs_send,
    rs_recv,
    z_send,
    z_recv,
    ex_send,
    ex_recv,
):
    rows, dl = tokens_ref.shape
    d_all = dl * 2
    half = dl // 2
    f = wg.shape[1]
    fs = sg.shape[1]
    chunk = zs * rows
    experts = zs * 4
    wide = slab.shape[3]

    me = lax.axis_index("ep")
    tp = lax.axis_index("tp")
    x, y, z = lax.rem(me, 2), lax.rem(me // 2, 2), me // 4
    own = y * 2 + x
    xcol = y * 2 + (1 - x)
    ycol = (1 - y) * 2 + x
    dcol = (1 - y) * 2 + (1 - x)
    x_dev = z * 4 + xcol
    y_dev = z * 4 + ycol
    zlist = [lax.rem(z + dz, zs) for dz in range(zs)]
    zdevs = [zi * 4 + own for zi in zlist]

    def ep_dev(e):
        return (e, tp)

    peer = (me, 1 - tp)
    pending = []

    def send(src, dst, ssem, rsem, dev):
        c = pltpu.make_async_remote_copy(
            src_ref=src,
            dst_ref=dst,
            send_sem=ssem,
            recv_sem=rsem,
            device_id=dev,
            device_id_type=pl.DeviceIdType.MESH,
        )
        c.start()
        pending.append(c)

    def landed(ref, rsem):
        pltpu.make_async_remote_copy(
            src_ref=ref,
            dst_ref=ref,
            send_sem=rsem,
            recv_sem=rsem,
            device_id=peer,
            device_id_type=pl.DeviceIdType.MESH,
        ).wait_recv()

    loads = []
    for i, (src, dst) in enumerate(
        (
            (sgate_hbm, sg),
            (sup_hbm, su),
            (gate_hbm.at[0], wg),
            (up_hbm.at[0], wu),
            (sdown_hbm, sd),
            (down_hbm.at[0], wd),
        )
    ):
        c = pltpu.make_async_copy(src, dst, w_sem.at[i])
        c.start()
        loads.append(c)

    barrier = pltpu.get_barrier_semaphore()
    others = [peer, ep_dev(x_dev), ep_dev(y_dev)] + [ep_dev(e) for e in zdevs[1:]]
    for dev in others:
        pl.semaphore_signal(barrier, inc=1, device_id=dev, device_id_type=pl.DeviceIdType.MESH)

    tok = tokens_ref[...].astype(F32)
    squares = jnp.sum(tok * tok, axis=1, keepdims=True)
    ss_s[0] = jnp.broadcast_to(squares, (rows, 128))
    lanes = lax.broadcasted_iota(jnp.int32, (rows, wide - dl), 1)
    wmat = jnp.zeros((rows, wide - dl), F32)
    wlow = jnp.zeros((rows, wide - dl), F32)
    for k in range(routes_ref.shape[1]):
        pick = routes_ref[:, k : k + 1]
        val = rw_ref[:, k : k + 1]
        high = val.astype(BF16).astype(F32)
        wmat = wmat + jnp.where(lanes == pick, high, 0.0)
        wlow = wlow + jnp.where(lanes == pick + experts, val - high, 0.0)
    slab[own, z, :, dl:wide] = (wmat + wlow).astype(BF16)

    pl.semaphore_wait(barrier, len(others))
    send(ss_s.at[0], ss_r.at[0], ex_send.at[0], ex_recv.at[0], peer)
    landed(ss_r.at[0], ex_recv.at[0])
    total = squares + ss_r[0][:, 0:1]
    normed = (tok * lax.rsqrt(total / d_all + 1e-06) * gain_ref[...]).astype(BF16)
    slab[own, z, :, 0:dl] = normed

    mine = slab.at[own, z]
    for dz in range(1, zs):
        send(mine, mine, ag_send.at[0, dz], ag_recv.at[0, z], ep_dev(zdevs[dz]))
    send(mine, mine, ag_send.at[1, 0], ag_recv.at[1, z], ep_dev(x_dev))
    send(mine, mine, ag_send.at[2, 0], ag_recv.at[2, z], ep_dev(y_dev))

    def relay_own(dz):
        zi = zlist[dz]
        ref = slab.at[own, zi]
        landed(ref, ag_recv.at[0, zi])
        send(ref, ref, ag_send.at[1, dz], ag_recv.at[1, zi], ep_dev(x_dev))
        send(ref, ref, ag_send.at[2, dz], ag_recv.at[2, zi], ep_dev(y_dev))

    low, high_part = pl.ds(0, half), pl.ds(half, wide - half)

    def relay_side(dz):
        zi = zlist[dz]
        landed(slab.at[xcol, zi], ag_recv.at[1, zi])
        ref = slab.at[xcol, zi, :, low]
        send(ref, ref, ag_send.at[3, dz], ag_recv.at[3, zi], ep_dev(y_dev))
        landed(slab.at[ycol, zi], ag_recv.at[2, zi])
        ref = slab.at[ycol, zi, :, high_part]
        send(ref, ref, ag_send.at[4, dz], ag_recv.at[4, zi], ep_dev(x_dev))

    def silu_mul(g, u):
        return (g / (1.0 + jnp.exp(-g)) * u).astype(BF16)

    loads[0].wait()
    loads[1].wait()
    tile = 256

    def shared_step(j, carry):
        cols = pl.ds(pl.multiple_of(j * tile, tile), tile)
        cols_up = pl.ds(pl.multiple_of(fs + j * tile, tile), tile)
        v = slab[own, z, :, 0:dl]
        sh_s[:, cols] = jnp.dot(v, sg[:, cols], preferred_element_type=F32).astype(BF16)
        sh_s[:, cols_up] = jnp.dot(v, su[:, cols], preferred_element_type=F32).astype(BF16)
        return carry

    lax.fori_loop(0, fs // tile, shared_step, 0)
    send(sh_s, sh_r, ex_send.at[1], ex_recv.at[1], peer)

    relay_own(1) if zs > 1 else None
    relay_side(0)

    landed(sh_r, ex_recv.at[1])
    loads[4].wait()
    sg_pre = sh_s[:, 0:fs].astype(F32) + sh_r[:, 0:fs].astype(F32)
    su_pre = sh_s[:, fs : 2 * fs].astype(F32) + sh_r[:, fs : 2 * fs].astype(F32)
    sh_hid = silu_mul(sg_pre, su_pre)
    for j in range(0, dl, 512):
        shared_out[:, j : j + 512] = jnp.dot(
            sh_hid, sd[:, j : j + 512], preferred_element_type=F32
        )

    for dz in range(2, zs):
        relay_own(dz)
        relay_side(dz - 1)

    loads[2].wait()
    loads[3].wait()

    def first(col, i):
        def step(j, carry):
            cols = pl.ds(pl.multiple_of(j * tile, tile), tile)
            cols_up = pl.ds(pl.multiple_of(f + j * tile, tile), tile)
            v = slab[col, :, :, 0:dl].reshape(chunk, dl)
            gu_s[i, :, cols] = jnp.dot(v, wg[:, cols], preferred_element_type=F32).astype(BF16)
            gu_s[i, :, cols_up] = jnp.dot(v, wu[:, cols], preferred_element_type=F32).astype(BF16)
            return carry

        lax.fori_loop(0, f // tile, step, 0)
        send(gu_s.at[i], gu_r.at[i], ex_send.at[2 + i], ex_recv.at[2 + i], peer)

    def second(col, i):
        landed(gu_r.at[i], ex_recv.at[2 + i])

        def act(j, carry):
            cols = pl.ds(pl.multiple_of(j * tile, tile), tile)
            cols_up = pl.ds(pl.multiple_of(f + j * tile, tile), tile)
            g = gu_s[i, :, cols].astype(F32) + gu_r[i, :, cols].astype(F32)
            u = gu_s[i, :, cols_up].astype(F32) + gu_r[i, :, cols_up].astype(F32)
            hid[:, cols] = silu_mul(g, u)
            return carry

        lax.fori_loop(0, f // tile, act, 0)
        wcols = slab[col, :, :, dl:wide].reshape(chunk, wide - dl).astype(F32)
        spots = lax.broadcasted_iota(jnp.int32, wcols.shape, 1)
        chosen = (spots == me) | (spots == me + experts)
        weight = jnp.sum(jnp.where(chosen, wcols, 0.0), axis=1, keepdims=True)

        def down(j, carry):
            cols = pl.ds(pl.multiple_of(j * tile, tile), tile)
            out = jnp.dot(hid[...], wd[:, cols], preferred_element_type=F32)
            obuf[:, cols] = out.astype(BF16).astype(F32) * weight
            return carry

        lax.fori_loop(0, dl // tile, down, 0)

    def shaped(v):
        return v.astype(BF16).reshape(zs, rows, half)

    X1, Y1, DA, DB, X2, Y2 = range(6)

    def rs(kind, dz, dev):
        zi = zlist[dz]
        send(
            sbuf.at[kind, zi], rbuf.at[kind, zi], rs_send.at[kind, zi], rs_recv.at[kind, zi], dev
        )

    def rs_landed(kind, dz):
        zi = zlist[dz]
        landed(rbuf.at[kind, zi], rs_recv.at[kind, zi])
        return rbuf[kind, zi].astype(F32)

    order = list(range(1, zs)) + [0]

    first(own, 0)
    relay_side(zs - 1) if zs > 1 else None
    loads[5].wait()
    second(own, 0)
    acc_o[...] = obuf[...].reshape(zs, rows, dl)
    first(xcol, 1)
    first(ycol, 2)
    second(xcol, 1)
    sbuf[X1] = shaped(obuf[:, half:dl])
    for dz in order:
        rs(X1, dz, ep_dev(x_dev))
    acc_x[...] = obuf[:, 0:half].reshape(zs, rows, half)
    second(ycol, 2)
    sbuf[Y1] = shaped(obuf[:, 0:half])
    for dz in order:
        rs(Y1, dz, ep_dev(y_dev))
    acc_y[...] = obuf[:, half:dl].reshape(zs, rows, half)
    for dz in range(zs):
        zi = zlist[dz]
        landed(slab.at[dcol, zi, :, low], ag_recv.at[3, zi])
        landed(slab.at[dcol, zi, :, high_part], ag_recv.at[4, zi])
    first(dcol, 3)
    second(dcol, 3)
    sbuf[DA] = shaped(obuf[:, 0:half])
    sbuf[DB] = shaped(obuf[:, half:dl])
    for dz in order:
        rs(DA, dz, ep_dev(y_dev))
        rs(DB, dz, ep_dev(x_dev))

    def middle(dz):
        zi = zlist[dz]
        sbuf[X2, zi] = (acc_x[zi] + rs_landed(DA, dz)).astype(BF16)
        rs(X2, dz, ep_dev(x_dev))
        sbuf[Y2, zi] = (acc_y[zi] + rs_landed(DB, dz)).astype(BF16)
        rs(Y2, dz, ep_dev(y_dev))

    def last(dz):
        zi = zlist[dz]
        left = acc_o[zi, :, 0:half] + rs_landed(Y1, dz) + rs_landed(X2, dz)
        right = acc_o[zi, :, half:dl] + rs_landed(X1, dz) + rs_landed(Y2, dz)
        if dz == 0:
            acc_o[zi, :, 0:half] = left
            acc_o[zi, :, half:dl] = right
        else:
            sz[dz, :, 0:half] = left.astype(BF16)
            sz[dz, :, half:dl] = right.astype(BF16)
            send(sz.at[dz], rz.at[z], z_send.at[dz], z_recv.at[z], ep_dev(zdevs[dz]))

    for n, dz in enumerate(order):
        middle(dz)
        if n > 0:
            last(order[n - 1])
    last(order[-1])

    mixed = shared_out[...] + acc_o[z]
    for dz in range(1, zs):
        zi = zlist[dz]
        landed(rz.at[zi], z_recv.at[zi])
        mixed = mixed + rz[zi].astype(F32)
    final = jnp.sum(mixed * mixed, axis=1, keepdims=True)
    ss_s[1] = jnp.broadcast_to(final, (rows, 128))
    send(ss_s.at[1], ss_r.at[1], ex_send.at[6], ex_recv.at[6], peer)
    landed(ss_r.at[1], ex_recv.at[6])
    final = final + ss_r[1][:, 0:1]
    out_ref[...] = (mixed * lax.rsqrt(final / d_all + 1e-06) * out_gain_ref[...]).astype(BF16)
    for c in pending:
        c.wait_send()


def fused(
    tokens,
    norm_gain,
    routes,
    route_weights,
    gate_proj,
    up_proj,
    down_proj,
    shared_gate,
    shared_up,
    shared_down,
    out_gain,
):
    rows, dl = tokens.shape
    ep = lax.axis_size("ep")
    zs = ep // 4
    f = gate_proj.shape[2]
    fs = shared_gate.shape[1]
    half = dl // 2
    chunk = zs * rows
    wide = dl + -(-2 * ep // 128) * 128
    vmem = pl.BlockSpec(memory_space=pltpu.VMEM)
    anys = pl.BlockSpec(memory_space=pl.ANY)
    dma = pltpu.SemaphoreType.DMA
    return pl.pallas_call(
        functools.partial(layer_kernel, zs),
        out_shape=jax.ShapeDtypeStruct((rows, dl), BF16),
        in_specs=[vmem] * 5 + [anys] * 6,
        out_specs=vmem,
        scratch_shapes=[
            pltpu.VMEM((dl, f), BF16),
            pltpu.VMEM((dl, f), BF16),
            pltpu.VMEM((f, dl), BF16),
            pltpu.VMEM((dl, fs), BF16),
            pltpu.VMEM((dl, fs), BF16),
            pltpu.VMEM((fs, dl), BF16),
            pltpu.VMEM((4, zs, rows, wide), BF16),
            pltpu.VMEM((4, chunk, 2 * f), BF16),
            pltpu.VMEM((4, chunk, 2 * f), BF16),
            pltpu.VMEM((rows, 2 * fs), BF16),
            pltpu.VMEM((rows, 2 * fs), BF16),
            pltpu.VMEM((2, rows, 128), F32),
            pltpu.VMEM((2, rows, 128), F32),
            pltpu.VMEM((6, zs, rows, half), BF16),
            pltpu.VMEM((6, zs, rows, half), BF16),
            pltpu.VMEM((zs, rows, dl), BF16),
            pltpu.VMEM((zs, rows, dl), BF16),
            pltpu.VMEM((zs, rows, half), F32),
            pltpu.VMEM((zs, rows, half), F32),
            pltpu.VMEM((zs, rows, dl), F32),
            pltpu.VMEM((chunk, dl), F32),
            pltpu.VMEM((rows, dl), F32),
            pltpu.VMEM((chunk, f), BF16),
            dma((6,)),
            dma((5, zs)),
            dma((5, zs)),
            dma((6, zs)),
            dma((6, zs)),
            dma((zs,)),
            dma((zs,)),
            dma((7,)),
            dma((7,)),
        ],
        compiler_params=pltpu.CompilerParams(
            collective_id=0, has_side_effects=True, vmem_limit_bytes=60 * 1024 * 1024
        ),
    )(
        tokens,
        norm_gain.reshape(1, dl),
        routes,
        route_weights,
        out_gain.reshape(1, dl),
        gate_proj,
        up_proj,
        down_proj,
        shared_gate,
        shared_up,
        shared_down,
    )


def per_device(
    tokens,
    norm_gain,
    routes,
    route_weights,
    gate_proj,
    up_proj,
    down_proj,
    shared_gate,
    shared_up,
    shared_down,
    out_gain,
):
    features = tokens.shape[1] * lax.axis_size("tp")
    tokens_f = tokens.astype(jnp.float32)
    squares = lax.psum(jnp.sum(tokens_f * tokens_f, axis=1), "tp")
    normed = (tokens_f * lax.rsqrt(squares / features + 1e-06)[:, None] * norm_gain[None, :]).astype(
        jnp.bfloat16
    )
    tok_rows, picks = routes.shape
    feat_local = tokens.shape[1]
    sources = lax.axis_size("ep")
    exp_local = gate_proj.shape[0]
    experts_all = sources * exp_local
    capacity = min(
        tok_rows, max(2, (3 * tok_rows * picks + 2 * experts_all - 1) // (2 * experts_all))
    )
    chosen = routes.reshape(-1)
    assigned = chosen.shape[0]
    earlier = jnp.arange(assigned)[None, :] < jnp.arange(assigned)[:, None]
    matches = (chosen[:, None] == chosen[None, :]) & earlier
    slot_rank = jnp.sum(matches.astype(jnp.int32), axis=1)
    slot_index = chosen * capacity + slot_rank
    source_rows = jnp.repeat(normed, picks, axis=0)
    outgoing = (
        jnp.zeros((experts_all * capacity, feat_local), jnp.bfloat16)
        .at[slot_index]
        .set(source_rows)
    )
    outgoing = outgoing.reshape(sources, exp_local, capacity, feat_local)
    arrived = lax.all_to_all(outgoing, "ep", split_axis=0, concat_axis=0, tiled=True)
    gate_part = jnp.einsum("sjcd,jdf->sjcf", arrived, gate_proj, preferred_element_type=jnp.float32)
    up_part = jnp.einsum("sjcd,jdf->sjcf", arrived, up_proj, preferred_element_type=jnp.float32)
    shared_gate_part = jnp.dot(normed, shared_gate, preferred_element_type=jnp.float32).reshape(
        1, 1, tok_rows, -1
    )
    shared_up_part = jnp.dot(normed, shared_up, preferred_element_type=jnp.float32).reshape(
        1, 1, tok_rows, -1
    )
    gate_pre, up_pre, shared_gate_pre, shared_up_pre = (
        lax.psum_scatter(
            gate_part.astype(jnp.bfloat16), "tp", scatter_dimension=3, tiled=True
        ).astype(jnp.float32),
        lax.psum_scatter(
            up_part.astype(jnp.bfloat16), "tp", scatter_dimension=3, tiled=True
        ).astype(jnp.float32),
        lax.psum_scatter(
            shared_gate_part.astype(jnp.bfloat16), "tp", scatter_dimension=3, tiled=True
        ).astype(jnp.float32),
        lax.psum_scatter(
            shared_up_part.astype(jnp.bfloat16), "tp", scatter_dimension=3, tiled=True
        ).astype(jnp.float32),
    )
    hidden_piece = (jax.nn.silu(gate_pre) * up_pre).astype(jnp.bfloat16)
    shared_piece = (jax.nn.silu(shared_gate_pre) * shared_up_pre).astype(jnp.bfloat16)
    hidden, shared_hidden = (
        lax.all_gather(hidden_piece, "tp", axis=3, tiled=True),
        lax.all_gather(shared_piece, "tp", axis=3, tiled=True),
    )
    expert_rows = jnp.einsum(
        "sjcf,jfd->sjcd", hidden, down_proj, preferred_element_type=jnp.float32
    ).astype(jnp.bfloat16)
    returned = lax.all_to_all(expert_rows, "ep", split_axis=0, concat_axis=0, tiled=True)
    returned = returned.reshape(experts_all * capacity, feat_local)
    gathered = returned[slot_index].astype(jnp.float32).reshape(tok_rows, picks, feat_local)
    routed = jnp.sum(gathered * route_weights[:, :, None], axis=1)
    shared_part = jnp.dot(
        shared_hidden.reshape(tok_rows, -1), shared_down, preferred_element_type=jnp.float32
    )
    mixed = shared_part + routed
    final_squares = lax.psum(jnp.sum(mixed * mixed, axis=1), "tp")
    return (mixed * lax.rsqrt(final_squares / features + 1e-06)[:, None] * out_gain[None, :]).astype(
        jnp.bfloat16
    )


def solution(mesh):
    one_chip_pair = mesh.shape["tp"] == 2 and mesh.shape["ep"] % 4 == 0

    def step(*args):
        fits = one_chip_pair and args[4].shape[0] == 1
        return (fused if fits else per_device)(*args)

    return jax.shard_map(
        step,
        mesh=mesh,
        in_specs=(
            P("ep", "tp"),
            P("tp"),
            P("ep", None),
            P("ep", None),
            P("ep", "tp", None),
            P("ep", "tp", None),
            P("ep", None, "tp"),
            P("tp", None),
            P("tp", None),
            P(None, "tp"),
            P("tp"),
        ),
        out_specs=P("ep", "tp"),
        check_vma=False,
    )
```

```python
import functools

import jax
import jax.numpy as jnp
from jax import lax
from jax.experimental import pallas as pl
from jax.experimental.pallas import tpu as pltpu
from jax.sharding import PartitionSpec as P


F32 = jnp.float32
BF16 = jnp.bfloat16


def layer_kernel(
    zs,
    tokens_ref,
    gain_ref,
    routes_ref,
    rw_ref,
    out_gain_ref,
    gate_hbm,
    up_hbm,
    down_hbm,
    sgate_hbm,
    sup_hbm,
    sdown_hbm,
    out_ref,
    wg,
    wu,
    wd,
    sg,
    su,
    sd,
    slab,
    gu_s,
    gu_r,
    sh_s,
    sh_r,
    ss_s,
    ss_r,
    sbuf,
    rbuf,
    sz,
    rz,
    acc_x,
    acc_y,
    acc_o,
    obuf,
    shared_out,
    hid,
    w_sem,
    ag_send,
    ag_recv,
    rs_send,
    rs_recv,
    z_send,
    z_recv,
    ex_send,
    ex_recv,
):
    rows, dl = tokens_ref.shape
    d_all = dl * 2
    half = dl // 2
    f = wg.shape[1]
    fs = sg.shape[1]
    chunk = zs * rows
    experts = zs * 4
    wide = slab.shape[3]

    me = lax.axis_index("ep")
    tp = lax.axis_index("tp")
    x, y, z = lax.rem(me, 2), lax.rem(me // 2, 2), me // 4
    own = y * 2 + x
    xcol = y * 2 + (1 - x)
    ycol = (1 - y) * 2 + x
    dcol = (1 - y) * 2 + (1 - x)
    x_dev = z * 4 + xcol
    y_dev = z * 4 + ycol
    zlist = [lax.rem(z + zs - dz, zs) for dz in range(zs)]
    zdevs = [zi * 4 + own for zi in zlist]

    def ep_dev(e):
        return (e, tp)

    peer = (me, 1 - tp)
    pending = []

    def send(src, dst, ssem, rsem, dev):
        c = pltpu.make_async_remote_copy(
            src_ref=src,
            dst_ref=dst,
            send_sem=ssem,
            recv_sem=rsem,
            device_id=dev,
            device_id_type=pl.DeviceIdType.MESH,
        )
        c.start()
        pending.append(c)

    def landed(ref, rsem):
        pltpu.make_async_remote_copy(
            src_ref=ref,
            dst_ref=ref,
            send_sem=rsem,
            recv_sem=rsem,
            device_id=peer,
            device_id_type=pl.DeviceIdType.MESH,
        ).wait_recv()

    loads = []
    for i, (src, dst) in enumerate(
        (
            (sgate_hbm, sg),
            (sup_hbm, su),
            (gate_hbm.at[0], wg),
            (up_hbm.at[0], wu),
            (sdown_hbm, sd),
            (down_hbm.at[0], wd),
        )
    ):
        c = pltpu.make_async_copy(src, dst, w_sem.at[i])
        c.start()
        loads.append(c)

    barrier = pltpu.get_barrier_semaphore()
    others = [peer, ep_dev(x_dev), ep_dev(y_dev)] + [ep_dev(e) for e in zdevs[1:]]
    for dev in others:
        pl.semaphore_signal(barrier, inc=1, device_id=dev, device_id_type=pl.DeviceIdType.MESH)

    tok = tokens_ref[...].astype(F32)
    squares = jnp.sum(tok * tok, axis=1, keepdims=True)
    ss_s[0] = jnp.broadcast_to(squares, (rows, 128))
    spread = (wide - dl, rows)
    names = lax.broadcasted_iota(jnp.int32, spread, 0)
    wmat = jnp.zeros(spread, F32)
    for k in range(routes_ref.shape[0]):
        pick = routes_ref[k : k + 1, :]
        val = rw_ref[k : k + 1, :]
        upper = val.astype(BF16).astype(F32)
        wmat = wmat + jnp.where(names == pick, upper, 0.0)
        wmat = wmat + jnp.where(names == pick + experts, val - upper, 0.0)
    square = (rows, rows)
    eye = (
        lax.broadcasted_iota(jnp.int32, square, 0) == lax.broadcasted_iota(jnp.int32, square, 1)
    ).astype(F32)
    slab[own, z, :, dl:wide] = lax.dot_general(
        eye.astype(BF16),
        wmat.astype(BF16),
        (((1,), (1,)), ((), ())),
        preferred_element_type=F32,
    ).astype(BF16)

    pl.semaphore_wait(barrier, len(others))
    send(ss_s.at[0], ss_r.at[0], ex_send.at[0], ex_recv.at[0], peer)
    landed(ss_r.at[0], ex_recv.at[0])
    total = squares + ss_r[0][:, 0:1]
    normed = (tok * lax.rsqrt(total / d_all + 1e-06) * gain_ref[...]).astype(BF16)
    slab[own, z, :, 0:dl] = normed

    mine = slab.at[own, z]
    for dz in range(1, zs):
        send(mine, mine, ag_send.at[0, dz], ag_recv.at[0, z], ep_dev(zdevs[zs - dz]))
    send(mine, mine, ag_send.at[1, 0], ag_recv.at[1, z], ep_dev(x_dev))
    send(mine, mine, ag_send.at[2, 0], ag_recv.at[2, z], ep_dev(y_dev))

    def relay_own(dz):
        zi = zlist[dz]
        ref = slab.at[own, zi]
        landed(ref, ag_recv.at[0, zi])
        send(ref, ref, ag_send.at[1, dz], ag_recv.at[1, zi], ep_dev(x_dev))
        send(ref, ref, ag_send.at[2, dz], ag_recv.at[2, zi], ep_dev(y_dev))

    low, high_part = pl.ds(0, half), pl.ds(half, wide - half)

    def relay_side(dz):
        zi = zlist[dz]
        landed(slab.at[xcol, zi], ag_recv.at[1, zi])
        ref = slab.at[xcol, zi, :, low]
        send(ref, ref, ag_send.at[3, dz], ag_recv.at[3, zi], ep_dev(y_dev))
        landed(slab.at[ycol, zi], ag_recv.at[2, zi])
        ref = slab.at[ycol, zi, :, high_part]
        send(ref, ref, ag_send.at[4, dz], ag_recv.at[4, zi], ep_dev(x_dev))

    def silu_mul(g, u):
        return (g / (1.0 + jnp.exp(-g)) * u).astype(BF16)

    loads[0].wait()
    loads[1].wait()
    tile = 256

    def shared_step(j, carry):
        cols = pl.ds(pl.multiple_of(j * tile, tile), tile)
        cols_up = pl.ds(pl.multiple_of(fs + j * tile, tile), tile)
        v = slab[own, z, :, 0:dl]
        sh_s[:, cols] = jnp.dot(v, sg[:, cols], preferred_element_type=F32).astype(BF16)
        sh_s[:, cols_up] = jnp.dot(v, su[:, cols], preferred_element_type=F32).astype(BF16)
        return carry

    lax.fori_loop(0, fs // tile, shared_step, 0)
    send(sh_s, sh_r, ex_send.at[1], ex_recv.at[1], peer)

    relay_own(1) if zs > 1 else None
    relay_side(0)

    for dz in range(2, zs):
        relay_own(dz)
        relay_side(dz - 1)

    loads[2].wait()
    loads[3].wait()

    pieces = gu_s.shape[1]
    part = f // pieces

    def first(col, i):
        for j in range(pieces):
            cols = slice(j * part, (j + 1) * part)
            v = slab[col, :, :, 0:dl].reshape(chunk, dl)
            g = jnp.dot(v, wg[:, cols], preferred_element_type=F32)
            gu_s[i, j, :, 0:part] = g.astype(BF16)
            u = jnp.dot(v, wu[:, cols], preferred_element_type=F32)
            gu_s[i, j, :, part : 2 * part] = u.astype(BF16)
            n = 3 + i * pieces + j
            send(gu_s.at[i, j], gu_r.at[i, j], ex_send.at[n], ex_recv.at[n], peer)

    def second(col, i):
        for j in range(pieces):
            landed(gu_r.at[i, j], ex_recv.at[3 + i * pieces + j])
            g = gu_s[i, j, :, 0:part].astype(F32) + gu_r[i, j, :, 0:part].astype(F32)
            u = gu_s[i, j, :, part:].astype(F32) + gu_r[i, j, :, part:].astype(F32)
            hid[:, j * part : (j + 1) * part] = silu_mul(g, u)
        wcols = slab[col, :, :, dl:wide].reshape(chunk, wide - dl).astype(F32)
        spots = lax.broadcasted_iota(jnp.int32, wcols.shape, 1)
        chosen = (spots == me) | (spots == me + experts)
        weight = jnp.sum(jnp.where(chosen, wcols, 0.0), axis=1, keepdims=True)

        step = min(512, dl)
        for j in range(0, dl, step):
            cols = slice(j, j + step)
            out = jnp.dot(hid[...], wd[:, cols], preferred_element_type=F32)
            obuf[:, cols] = out.astype(BF16).astype(F32) * weight

    def shaped(v):
        return v.astype(BF16).reshape(zs, rows, half)

    X1, Y1, DA, DB, X2, Y2 = range(6)

    def rs(kind, dz, dev):
        zi = zlist[dz]
        send(
            sbuf.at[kind, zi], rbuf.at[kind, zi], rs_send.at[kind, zi], rs_recv.at[kind, zi], dev
        )

    def rs_landed(kind, dz):
        zi = zlist[dz]
        landed(rbuf.at[kind, zi], rs_recv.at[kind, zi])
        return rbuf[kind, zi].astype(F32)

    order = list(range(1, zs)) + [0]

    first(own, 0)
    relay_side(zs - 1) if zs > 1 else None
    loads[5].wait()
    first(xcol, 1)
    first(ycol, 2)
    second(xcol, 1)
    sbuf[X1] = shaped(obuf[:, half:dl])
    for dz in order:
        rs(X1, dz, ep_dev(x_dev))
    acc_x[...] = obuf[:, 0:half].reshape(zs, rows, half)
    second(ycol, 2)
    sbuf[Y1] = shaped(obuf[:, 0:half])
    for dz in order:
        rs(Y1, dz, ep_dev(y_dev))
    acc_y[...] = obuf[:, half:dl].reshape(zs, rows, half)
    for dz in range(zs):
        zi = zlist[dz]
        landed(slab.at[dcol, zi, :, low], ag_recv.at[3, zi])
        landed(slab.at[dcol, zi, :, high_part], ag_recv.at[4, zi])
    first(dcol, 3)
    second(dcol, 3)
    sbuf[DA] = shaped(obuf[:, 0:half])
    sbuf[DB] = shaped(obuf[:, half:dl])
    for dz in order:
        rs(DA, dz, ep_dev(y_dev))
        rs(DB, dz, ep_dev(x_dev))

    second(own, 0)
    acc_o[...] = obuf[...].reshape(zs, rows, dl)
    landed(sh_r, ex_recv.at[1])
    loads[4].wait()
    sg_pre = sh_s[:, 0:fs].astype(F32) + sh_r[:, 0:fs].astype(F32)
    su_pre = sh_s[:, fs : 2 * fs].astype(F32) + sh_r[:, fs : 2 * fs].astype(F32)
    sh_hid = silu_mul(sg_pre, su_pre)
    for j in range(0, dl, 512):
        shared_out[:, j : j + 512] = jnp.dot(
            sh_hid, sd[:, j : j + 512], preferred_element_type=F32
        )

    def middle(dz):
        zi = zlist[dz]
        sbuf[X2, zi] = (acc_x[zi] + rs_landed(DA, dz)).astype(BF16)
        rs(X2, dz, ep_dev(x_dev))
        sbuf[Y2, zi] = (acc_y[zi] + rs_landed(DB, dz)).astype(BF16)
        rs(Y2, dz, ep_dev(y_dev))

    def last(dz):
        zi = zlist[dz]
        left = acc_o[zi, :, 0:half] + rs_landed(Y1, dz) + rs_landed(X2, dz)
        right = acc_o[zi, :, half:dl] + rs_landed(X1, dz) + rs_landed(Y2, dz)
        if dz == 0:
            acc_o[zi, :, 0:half] = left
            acc_o[zi, :, half:dl] = right
        else:
            sz[dz, :, 0:half] = left.astype(BF16)
            sz[dz, :, half:dl] = right.astype(BF16)
            send(sz.at[dz], rz.at[z], z_send.at[dz], z_recv.at[z], ep_dev(zdevs[dz]))

    for n, dz in enumerate(order):
        middle(dz)
        if n > 0:
            last(order[n - 1])
    last(order[-1])

    mixed = shared_out[...] + acc_o[z]
    for dz in range(1, zs):
        zi = zlist[dz]
        landed(rz.at[zi], z_recv.at[zi])
        mixed = mixed + rz[zi].astype(F32)
    final = jnp.sum(mixed * mixed, axis=1, keepdims=True)
    ss_s[1] = jnp.broadcast_to(final, (rows, 128))
    send(ss_s.at[1], ss_r.at[1], ex_send.at[2], ex_recv.at[2], peer)
    landed(ss_r.at[1], ex_recv.at[2])
    final = final + ss_r[1][:, 0:1]
    out_ref[...] = (mixed * lax.rsqrt(final / d_all + 1e-06) * out_gain_ref[...]).astype(BF16)
    for c in pending:
        c.wait_send()


def fused(
    tokens,
    norm_gain,
    routes,
    route_weights,
    gate_proj,
    up_proj,
    down_proj,
    shared_gate,
    shared_up,
    shared_down,
    out_gain,
):
    rows, dl = tokens.shape
    ep = lax.axis_size("ep")
    zs = ep // 4
    f = gate_proj.shape[2]
    fs = shared_gate.shape[1]
    half = dl // 2
    chunk = zs * rows
    wide = dl + -(-2 * ep // 128) * 128
    pieces = max(1, f // 512)
    vmem = pl.BlockSpec(memory_space=pltpu.VMEM)
    anys = pl.BlockSpec(memory_space=pl.ANY)
    dma = pltpu.SemaphoreType.DMA
    return pl.pallas_call(
        functools.partial(layer_kernel, zs),
        out_shape=jax.ShapeDtypeStruct((rows, dl), BF16),
        in_specs=[vmem] * 5 + [anys] * 6,
        out_specs=vmem,
        scratch_shapes=[
            pltpu.VMEM((dl, f), BF16),
            pltpu.VMEM((dl, f), BF16),
            pltpu.VMEM((f, dl), BF16),
            pltpu.VMEM((dl, fs), BF16),
            pltpu.VMEM((dl, fs), BF16),
            pltpu.VMEM((fs, dl), BF16),
            pltpu.VMEM((4, zs, rows, wide), BF16),
            pltpu.VMEM((4, pieces, chunk, 2 * f // pieces), BF16),
            pltpu.VMEM((4, pieces, chunk, 2 * f // pieces), BF16),
            pltpu.VMEM((rows, 2 * fs), BF16),
            pltpu.VMEM((rows, 2 * fs), BF16),
            pltpu.VMEM((2, rows, 128), F32),
            pltpu.VMEM((2, rows, 128), F32),
            pltpu.VMEM((6, zs, rows, half), BF16),
            pltpu.VMEM((6, zs, rows, half), BF16),
            pltpu.VMEM((zs, rows, dl), BF16),
            pltpu.VMEM((zs, rows, dl), BF16),
            pltpu.VMEM((zs, rows, half), F32),
            pltpu.VMEM((zs, rows, half), F32),
            pltpu.VMEM((zs, rows, dl), F32),
            pltpu.VMEM((chunk, dl), F32),
            pltpu.VMEM((rows, dl), F32),
            pltpu.VMEM((chunk, f), BF16),
            dma((6,)),
            dma((5, zs)),
            dma((5, zs)),
            dma((6, zs)),
            dma((6, zs)),
            dma((zs,)),
            dma((zs,)),
            dma((3 + 4 * pieces,)),
            dma((3 + 4 * pieces,)),
        ],
        compiler_params=pltpu.CompilerParams(
            collective_id=0, has_side_effects=True, vmem_limit_bytes=60 * 1024 * 1024
        ),
    )(
        tokens,
        norm_gain.reshape(1, dl),
        routes.T,
        route_weights.T,
        out_gain.reshape(1, dl),
        gate_proj,
        up_proj,
        down_proj,
        shared_gate,
        shared_up,
        shared_down,
    )


def per_device(
    tokens,
    norm_gain,
    routes,
    route_weights,
    gate_proj,
    up_proj,
    down_proj,
    shared_gate,
    shared_up,
    shared_down,
    out_gain,
):
    features = tokens.shape[1] * lax.axis_size("tp")
    tokens_f = tokens.astype(jnp.float32)
    squares = lax.psum(jnp.sum(tokens_f * tokens_f, axis=1), "tp")
    normed = (tokens_f * lax.rsqrt(squares / features + 1e-06)[:, None] * norm_gain[None, :]).astype(
        jnp.bfloat16
    )
    tok_rows, picks = routes.shape
    feat_local = tokens.shape[1]
    sources = lax.axis_size("ep")
    exp_local = gate_proj.shape[0]
    experts_all = sources * exp_local
    capacity = min(
        tok_rows, max(2, (3 * tok_rows * picks + 2 * experts_all - 1) // (2 * experts_all))
    )
    chosen = routes.reshape(-1)
    assigned = chosen.shape[0]
    earlier = jnp.arange(assigned)[None, :] < jnp.arange(assigned)[:, None]
    matches = (chosen[:, None] == chosen[None, :]) & earlier
    slot_rank = jnp.sum(matches.astype(jnp.int32), axis=1)
    slot_index = chosen * capacity + slot_rank
    source_rows = jnp.repeat(normed, picks, axis=0)
    outgoing = (
        jnp.zeros((experts_all * capacity, feat_local), jnp.bfloat16)
        .at[slot_index]
        .set(source_rows)
    )
    outgoing = outgoing.reshape(sources, exp_local, capacity, feat_local)
    arrived = lax.all_to_all(outgoing, "ep", split_axis=0, concat_axis=0, tiled=True)
    gate_part = jnp.einsum("sjcd,jdf->sjcf", arrived, gate_proj, preferred_element_type=jnp.float32)
    up_part = jnp.einsum("sjcd,jdf->sjcf", arrived, up_proj, preferred_element_type=jnp.float32)
    shared_gate_part = jnp.dot(normed, shared_gate, preferred_element_type=jnp.float32).reshape(
        1, 1, tok_rows, -1
    )
    shared_up_part = jnp.dot(normed, shared_up, preferred_element_type=jnp.float32).reshape(
        1, 1, tok_rows, -1
    )
    gate_pre, up_pre, shared_gate_pre, shared_up_pre = (
        lax.psum_scatter(
            gate_part.astype(jnp.bfloat16), "tp", scatter_dimension=3, tiled=True
        ).astype(jnp.float32),
        lax.psum_scatter(
            up_part.astype(jnp.bfloat16), "tp", scatter_dimension=3, tiled=True
        ).astype(jnp.float32),
        lax.psum_scatter(
            shared_gate_part.astype(jnp.bfloat16), "tp", scatter_dimension=3, tiled=True
        ).astype(jnp.float32),
        lax.psum_scatter(
            shared_up_part.astype(jnp.bfloat16), "tp", scatter_dimension=3, tiled=True
        ).astype(jnp.float32),
    )
    hidden_piece = (jax.nn.silu(gate_pre) * up_pre).astype(jnp.bfloat16)
    shared_piece = (jax.nn.silu(shared_gate_pre) * shared_up_pre).astype(jnp.bfloat16)
    hidden, shared_hidden = (
        lax.all_gather(hidden_piece, "tp", axis=3, tiled=True),
        lax.all_gather(shared_piece, "tp", axis=3, tiled=True),
    )
    expert_rows = jnp.einsum(
        "sjcf,jfd->sjcd", hidden, down_proj, preferred_element_type=jnp.float32
    ).astype(jnp.bfloat16)
    returned = lax.all_to_all(expert_rows, "ep", split_axis=0, concat_axis=0, tiled=True)
    returned = returned.reshape(experts_all * capacity, feat_local)
    gathered = returned[slot_index].astype(jnp.float32).reshape(tok_rows, picks, feat_local)
    routed = jnp.sum(gathered * route_weights[:, :, None], axis=1)
    shared_part = jnp.dot(
        shared_hidden.reshape(tok_rows, -1), shared_down, preferred_element_type=jnp.float32
    )
    mixed = shared_part + routed
    final_squares = lax.psum(jnp.sum(mixed * mixed, axis=1), "tp")
    return (mixed * lax.rsqrt(final_squares / features + 1e-06)[:, None] * out_gain[None, :]).astype(
        jnp.bfloat16
    )


def solution(mesh):
    one_chip_pair = mesh.shape["tp"] == 2 and mesh.shape["ep"] % 4 == 0

    def step(*args):
        fits = one_chip_pair and args[4].shape[0] == 1
        return (fused if fits else per_device)(*args)

    return jax.shard_map(
        step,
        mesh=mesh,
        in_specs=(
            P("ep", "tp"),
            P("tp"),
            P("ep", None),
            P("ep", None),
            P("ep", "tp", None),
            P("ep", "tp", None),
            P("ep", None, "tp"),
            P("tp", None),
            P("tp", None),
            P(None, "tp"),
            P("tp"),
        ),
        out_specs=P("ep", "tp"),
        check_vma=False,
    )
```
